32 devices in a mesh: fs: 4 (over z), tp: 4 (over y, x), rep: 2 (over core).
Axes of the slice: x: 2, y: 2, z: 4, core: 2. Of those that a mesh axis runs over, the one named last changes fastest.
Arguments:
- up_weight: float32 [2048, 8192], P('fs', ('tp', 'rep')), may hold values from -0.125 to 0.125
- up_momentum: float32 [2048, 8192], P('fs', ('tp', 'rep')), may hold values from -24 to 24
- up_grads: bfloat16 [2, 2048, 8192], P('rep', 'fs', 'tp'), may hold values from -2.09375 to 2.09375
- out_weight: float32 [2048, 2048], P('fs', ('tp', 'rep')), may hold values from -0.125 to 0.125
- out_momentum: float32 [2048, 2048], P('fs', ('tp', 'rep')), may hold values from -24 to 24
- out_grads: bfloat16 [2, 2048, 2048], P('rep', 'fs', 'tp'), may hold values from -2.09375 to 2.09375
Outputs:
- up_weight_new: float32 [2048, 8192], P('fs', ('tp', 'rep'))
- up_momentum_new: float32 [2048, 8192], P('fs', ('tp', 'rep'))
- up_direction: float32 [2048, 8192], P('fs', ('tp', 'rep'))
- out_weight_new: float32 [2048, 2048], P('fs', ('tp', 'rep'))
- out_momentum_new: float32 [2048, 2048], P('fs', ('tp', 'rep'))
- out_direction: float32 [2048, 2048], P('fs', ('tp', 'rep'))
The draws below stay inside these ranges and needn't reach their ends.
All inputs are finite; a program needn't handle non-finite values.
Results may differ from the reference program's by a relative error of at most 0.039.
Values may be sent and summed in bfloat16 or wider, within the bound.
A program may use at most 64 MiB of HBM per device.

```python
import math
import jax
import jax.numpy as jnp
from jax import lax

D = 2048
FF = 8192
DMIX = 2048
ITERS = 3
N_REP = 2


def spread_rows(key, row_count, width):
    keys = jax.random.split(key, 4)
    base = jax.random.normal(keys[0], (row_count, width), jnp.float32)
    base = jnp.clip(base, -5.5, 5.5)
    group_rows = row_count // 16
    group_scale = jnp.exp(jax.random.uniform(keys[1], (16,), jnp.float32, math.log(0.12), math.log(3.0)))
    row_scale = jnp.exp(jax.random.uniform(keys[2], (row_count,), jnp.float32, math.log(0.7), math.log(1.4)))
    scale = group_scale[jnp.arange(row_count) // group_rows] * row_scale
    return base * scale[:, None]


def draw_up_momentum(key, part):
    return spread_rows(jax.random.fold_in(key, 11), D, FF)


def draw_out_momentum(key, part):
    return spread_rows(jax.random.fold_in(key, 23), DMIX, D)


def level_of(stream_key, shape, pieces, least, top_value):
    def one(position, parts):
        steps = jax.random.uniform(jax.random.fold_in(jax.random.fold_in(stream_key, 6), position), (parts,), jnp.float32, least / len(pieces), top_value / len(pieces))
        return jnp.repeat(jnp.exp(steps), shape[position] // parts).reshape((-1,) + (1,) * (len(shape) - position - 1))

    loudness = one(*pieces[0])
    for cut in pieces[1:]:
        loudness = loudness * one(*cut)
    return loudness


def scatter_about(rng, extent, deviation, most, shards=(), kind=jnp.bfloat16):
    gain = level_of(rng, extent, shards, -0.22, 0.18) if shards else 1.0
    values = jax.random.normal(rng, extent, jnp.float32) * deviation * gain
    return jnp.minimum(jnp.maximum(values, -most), most).astype(kind)


def setup_inputs(seed: int = 0) -> dict:
    arg_keys = jax.random.split(jax.random.key(seed), 7)
    up_weight = scatter_about(arg_keys[0], (D, FF), D ** -0.5, 0.125, ((0, 4), (1, 8)), jnp.float32)
    up_momentum = draw_up_momentum(jax.random.fold_in(arg_keys[6], 71), 0)
    up_grads = scatter_about(arg_keys[2], (N_REP, D, FF), 0.35, 2.09375, ((0, 2), (1, 4), (2, 4)))
    out_weight = scatter_about(arg_keys[3], (DMIX, D), DMIX ** -0.5, 0.125, ((0, 4), (1, 8)), jnp.float32)
    out_momentum = draw_out_momentum(jax.random.fold_in(arg_keys[6], 71), 0)
    out_grads = scatter_about(arg_keys[5], (N_REP, DMIX, D), 0.35, 2.09375, ((0, 2), (1, 4), (2, 4)))
    return dict(up_weight=up_weight, up_momentum=up_momentum, up_grads=up_grads, out_weight=out_weight, out_momentum=out_momentum, out_grads=out_grads)


MOMENT = 0.9
RATE = 0.02
COEF_A = 3.4445
COEF_B = -4.775
COEF_C = 2.0315

def orthogonal(moment):
    current = moment
    for iteration in range(ITERS):
        values = current.astype(jnp.bfloat16)
        gram = jnp.dot(values, values.T, preferred_element_type=jnp.float32)
        if iteration == 0:
            square = 1.0 / (jnp.sqrt(jnp.sum(gram * gram)) + 1.0)
            factor = jnp.sqrt(square)
        else:
            square = 1.0
            factor = 1.0
        halved = (gram * square).astype(jnp.bfloat16)
        product = factor * jnp.dot(halved, values, preferred_element_type=jnp.float32)
        second = jnp.dot(halved, product.astype(jnp.bfloat16), preferred_element_type=jnp.float32)
        current = COEF_A * factor * current + COEF_B * product + COEF_C * second
    return current

def update(weight, momentum, grads):
    grad = lax.optimization_barrier(jnp.sum(grads.astype(jnp.float32), axis=0))
    moment = MOMENT * momentum + grad
    direction = orthogonal(moment) * math.sqrt(momentum.shape[1])
    return (weight - RATE * direction, moment, direction)

def reference(up_weight, up_momentum, up_grads, out_weight, out_momentum, out_grads):
    up_new, up_moment, up_step = update(up_weight, up_momentum, up_grads)
    out_new, out_moment, out_step = update(out_weight, out_momentum, out_grads)
    return (up_new, up_moment, up_step, out_new, out_moment, out_step)
```

```python
import functools
import math

import jax
import jax.numpy as jnp
from jax import lax
from jax.experimental import pallas as pl
from jax.experimental.pallas import tpu as pltpu
from jax.sharding import PartitionSpec as P

ITERS = 3
MOMENT = 0.9
RATE = 0.02
COEF_A = 3.4445
COEF_B = -4.775
COEF_C = 2.0315
BF = jnp.bfloat16
F32 = jnp.float32
CUTS = 8
PANELS = 4


def mm(a, b):
    return jnp.dot(a, b, preferred_element_type=F32)


def mm_t(a, b):
    return lax.dot_general(a, b, (((1,), (1,)), ((), ())), preferred_element_type=F32)


def reduced_grad(grads):
    size = lax.axis_size("rep")
    rows, cols = grads.shape
    pieces = grads.reshape(rows, size, cols // size).transpose(1, 0, 2)
    pieces = lax.all_to_all(pieces, "rep", split_axis=0, concat_axis=0, tiled=True)
    return jnp.sum(pieces.astype(F32), axis=0)


def to_columns(values):
    size = lax.axis_size("fs")
    rows, cols = values.shape
    pieces = values.reshape(rows, size, cols // size).transpose(1, 0, 2)
    pieces = lax.all_to_all(pieces, "fs", split_axis=0, concat_axis=0, tiled=True)
    return pieces.reshape(size * rows, cols // size)


def to_rows(values):
    size = lax.axis_size("fs")
    rows, cols = values.shape
    pieces = values.reshape(size, rows // size, cols)
    pieces = lax.all_to_all(pieces, "fs", split_axis=0, concat_axis=0, tiled=True)
    return pieces.transpose(1, 0, 2).reshape(rows // size, cols * size)


def swap_pairs(values):
    size = lax.axis_size("rep")
    return lax.ppermute(values, "rep", [(i, i ^ 1) for i in range(size)])


def blocks_of(cuts):
    return [(i, j) for i in range(cuts) for j in range(i, cuts)]


def gram_kernel(x_ref, o_ref):
    step = x_ref.shape[0] // CUTS
    span = CUTS // PANELS
    place = {pair: k for k, pair in enumerate(blocks_of(CUTS))}
    for p in range(PANELS):
        low = p * span
        rows = x_ref[low * step : (low + span) * step, :]
        value = mm_t(rows, x_ref[low * step :, :]).astype(BF)
        for i in range(span):
            for j in range(low + i, CUTS):
                k = place[low + i, j]
                o_ref[k * step : (k + 1) * step, :] = value[
                    i * step : (i + 1) * step, (j - low) * step : (j - low + 1) * step
                ]


def gram(x):
    size, width = x.shape
    step = size // CUTS
    count = len(blocks_of(CUTS))
    return pl.pallas_call(
        gram_kernel,
        name="gram",
        out_shape=jax.ShapeDtypeStruct((count * step, step), BF),
        in_specs=[pl.BlockSpec(memory_space=pltpu.VMEM)],
        out_specs=pl.BlockSpec(memory_space=pltpu.VMEM),
        compiler_params=pltpu.CompilerParams(vmem_limit_bytes=48 << 20),
        cost_estimate=pl.CostEstimate(
            flops=2 * width * count * step * step, bytes_accessed=2 * size * width, transcendentals=0
        ),
    )(x)


S1X, S1Y, S2X0, S2X1, S2Y0, S2Y1, RZ, AZ, AX, AY, AD0, AD1 = range(12)


def reduce_kernel(planes, g_ref, o_ref, first, second, mixed, third, moved, own, send, recv):
    z, t, r = lax.axis_index("fs"), lax.axis_index("tp"), lax.axis_index("rep")
    half = g_ref.shape[1] // 2
    parts = (pl.ds(0, half), pl.ds(half, half))
    beside, above, corner = t ^ 1, t ^ 2, t ^ 3
    to_x, to_y = (z, beside, r), (z, above, r)
    others = list(range(1, planes))
    order = others + [0]

    barrier = pltpu.get_barrier_semaphore()
    peers = [to_x, to_y] + [(z ^ m, t, r) for m in others]
    for peer in peers:
        pl.semaphore_signal(barrier, inc=1, device_id=peer, device_id_type=pl.DeviceIdType.MESH)
    pl.semaphore_wait(barrier, len(peers))

    def chunk(m, s):
        return (z ^ m) * 4 + s

    started = []

    def copy(kind, m, src, dst, peer, start=True):
        c = pltpu.make_async_remote_copy(
            src_ref=src,
            dst_ref=dst,
            send_sem=send.at[kind, m],
            recv_sem=recv.at[kind, m],
            device_id=peer,
            device_id_type=pl.DeviceIdType.MESH,
        )
        if start:
            c.start()
            started.append(c)
        return c

    def arrived(kind, m, dst):
        copy(kind, m, dst, dst, to_x, start=False).wait_recv()

    def corner_halves(m):
        copy(S1Y, m, g_ref.at[chunk(m, corner), parts[0]], first.at[m, 0], to_y)
        copy(S1X, m, g_ref.at[chunk(m, corner), parts[1]], first.at[m, 1], to_x)

    def direct_halves(m):
        copy(S2X1, m, g_ref.at[chunk(m, beside), parts[1]], second.at[m, 0, parts[1]], to_x)
        copy(S2Y0, m, g_ref.at[chunk(m, above), parts[0]], second.at[m, 1, parts[0]], to_y)

    corner_halves(order[0])
    corner_halves(order[1])
    direct_halves(order[0])
    for k in range(planes + 1):
        if k < planes:
            m = order[k]
            arrived(S1Y, m, first.at[m, 0])
            mixed[m, 0] = (g_ref[chunk(m, beside), parts[0]].astype(F32) + first[m, 0].astype(F32)).astype(BF)
            copy(S2X0, m, mixed.at[m, 0], second.at[m, 0, parts[0]], to_x)
            arrived(S1X, m, first.at[m, 1])
            mixed[m, 1] = (g_ref[chunk(m, above), parts[1]].astype(F32) + first[m, 1].astype(F32)).astype(BF)
            copy(S2Y1, m, mixed.at[m, 1], second.at[m, 1, parts[1]], to_y)
            if k + 2 < planes:
                corner_halves(order[k + 2])
            if k + 1 < planes:
                direct_halves(order[k + 1])
        if k >= 1:
            m = order[k - 1]
            arrived(S2X1, m, second.at[m, 0, parts[1]])
            arrived(S2Y0, m, second.at[m, 1, parts[0]])
            arrived(S2X0, m, second.at[m, 0, parts[0]])
            arrived(S2Y1, m, second.at[m, 1, parts[1]])
            value = g_ref[chunk(m, t)].astype(F32) + second[m, 0].astype(F32) + second[m, 1].astype(F32)
            if m:
                moved[m] = value.astype(BF)
                copy(RZ, m, moved.at[m], third.at[m], (z ^ m, t, r))
            else:
                own[...] = value
    value = own[...]
    for m in others:
        arrived(RZ, m, third.at[m])
        value = value + third[m].astype(F32)
    o_ref[chunk(0, t)] = value.astype(BF)

    def to_neighbours(m):
        copy(AX, m, o_ref.at[chunk(m, t)], o_ref.at[chunk(m, t)], to_x)
        copy(AY, m, o_ref.at[chunk(m, t)], o_ref.at[chunk(m, t)], to_y)

    def to_corner(m):
        arrived(AX, m, o_ref.at[chunk(m, beside)])
        copy(AD0, m, o_ref.at[chunk(m, beside), parts[0]], o_ref.at[chunk(m, beside), parts[0]], to_y)
        arrived(AY, m, o_ref.at[chunk(m, above)])
        copy(AD1, m, o_ref.at[chunk(m, above), parts[1]], o_ref.at[chunk(m, above), parts[1]], to_x)

    to_neighbours(0)
    for m in others:
        copy(AZ, m, o_ref.at[chunk(0, t)], o_ref.at[chunk(0, t)], (z ^ m, t, r))
    before = 0
    for m in others:
        arrived(AZ, m, o_ref.at[chunk(m, t)])
        to_neighbours(m)
        to_corner(before)
        before = m
    to_corner(before)
    for m in [0] + others:
        arrived(AD0, m, o_ref.at[chunk(m, corner), parts[0]])
        arrived(AD1, m, o_ref.at[chunk(m, corner), parts[1]])
    for c in started:
        c.wait_send()


def reduced(packed):
    planes = lax.axis_size("fs")
    chunks = planes * 4
    rows, width = packed.shape
    size = rows // chunks
    out = pl.pallas_call(
        functools.partial(reduce_kernel, planes),
        name="reduced",
        out_shape=jax.ShapeDtypeStruct((chunks, size, width), BF),
        in_specs=[pl.BlockSpec(memory_space=pltpu.VMEM)],
        out_specs=pl.BlockSpec(memory_space=pltpu.VMEM),
        scratch_shapes=[
            pltpu.VMEM((planes, 2, size // 2, width), BF),
            pltpu.VMEM((planes, 2, size, width), BF),
            pltpu.VMEM((planes, 2, size // 2, width), BF),
            pltpu.VMEM((planes, size, width), BF),
            pltpu.VMEM((planes, size, width), BF),
            pltpu.VMEM((size, width), F32),
            pltpu.SemaphoreType.DMA((12, planes)),
            pltpu.SemaphoreType.DMA((12, planes)),
        ],
        compiler_params=pltpu.CompilerParams(
            collective_id=1, has_side_effects=True, vmem_limit_bytes=48 << 20
        ),
    )(packed.reshape(chunks, size, width))
    return out.reshape(rows, width)


def total_gram(packed):
    fs, tp, rep = (lax.axis_size(name) for name in ("fs", "tp", "rep"))
    if rep == 2 and tp == 4 and fs & (fs - 1) == 0 and packed.shape[0] % (fs * tp * 32) == 0:
        return reduced(packed)
    packed = lax.psum(packed, ("fs", "tp"))
    if rep > 2:
        groups = [[i for i in range(rep) if i % 2 == k] for k in range(2)]
        packed = lax.psum(packed, "rep", axis_index_groups=groups)
    return packed


def unpack(packed, mats):
    step = packed.shape[1]
    pairs = blocks_of(CUTS)
    total = jnp.zeros((step, step), F32)
    for k, (i, j) in enumerate(pairs):
        value = packed[k * step : (k + 1) * step, :].astype(F32)
        total = total + (value * value if i == j else 2.0 * (value * value))
    square = 1.0 / (jnp.sqrt(jnp.sum(total, keepdims=True)) + 1.0)
    for k, (i, j) in enumerate(pairs):
        value = (packed[k * step : (k + 1) * step, :].astype(F32) * square).astype(BF)
        mats[0, i * step : (i + 1) * step, j * step : (j + 1) * step] = value
        if i != j:
            mats[0, j * step : (j + 1) * step, i * step : (i + 1) * step] = value.T
    return jnp.sqrt(square)


def symmetric_step(mats, left, right, out, alpha, beta):
    size = mats.shape[1]
    step = size // PANELS
    for i in range(PANELS):
        low, high = i * step, (i + 1) * step
        product = mm(mats[left, low:high, :], mats[right, :, low:])
        value = (alpha * mats[right, low:high, low:].astype(F32) + beta * product).astype(BF)
        mats[out, low:high, low:] = value
        for j in range(i + 1, PANELS):
            mats[out, j * step : (j + 1) * step, low:high] = value[:, (j - i) * step : (j - i + 1) * step].T


def thin_step(mats, index, vals, source, target, alpha):
    size = mats.shape[1]
    step = size // PANELS

    def panel(i, _):
        rows = pl.ds(pl.multiple_of(i * step, step), step)
        product = mm(mats[index, rows, :], vals[source])
        vals[target, rows, :] = (alpha * vals[source, rows, :].astype(F32) + product).astype(BF)
        return 0

    lax.fori_loop(0, PANELS, panel, 0)


def chain_kernel(g_ref, v_ref, o_ref, mats, vals):
    factor = unpack(g_ref, mats)
    vals[0] = v_ref[...]

    def product(k, _):
        left = jnp.where(k == 0, 0, 1)
        right = jnp.where(k == 2, 2, 0)
        out = jnp.where(k == 0, 1, jnp.where(k == 1, 2, 0))
        alpha = jnp.where(k == 0, COEF_B, COEF_A).astype(F32)
        beta = jnp.where(k == 0, COEF_C, 1.0).astype(F32)
        symmetric_step(mats, left, right, out, alpha, beta)
        return 0

    def iteration(t, _):
        lax.fori_loop(0, 3, product, 0)
        thin_step(mats, 1, vals, t, t + 1, COEF_A)
        return 0

    lax.fori_loop(0, ITERS - 1, iteration, 0)
    size = mats.shape[1]
    step = size // PANELS
    last = ITERS - 1
    for source, target in ((last, 0), (0, 1)):
        def panel(i, _):
            rows = pl.ds(pl.multiple_of(i * step, step), step)
            product = mm(mats[0, rows, :], vals[source])
            if target == 0:
                vals[0, rows, :] = product.astype(BF)
            else:
                value = COEF_A * vals[last, rows, :].astype(F32) + COEF_B * vals[0, rows, :].astype(F32)
                o_ref[rows, :] = (factor * (value + COEF_C * product)).astype(BF)
            return 0
        lax.fori_loop(0, PANELS, panel, 0)


def chain(packed, v):
    size, width = v.shape
    flops = 2 * size * size * (4 * width + 6 * size * 5 // 8)
    return pl.pallas_call(
        chain_kernel,
        name="chain",
        out_shape=jax.ShapeDtypeStruct(v.shape, BF),
        in_specs=[pl.BlockSpec(memory_space=pltpu.VMEM)] * 2,
        out_specs=pl.BlockSpec(memory_space=pltpu.VMEM),
        scratch_shapes=[pltpu.VMEM((3, size, size), BF), pltpu.VMEM((ITERS, size, width), BF)],
        compiler_params=pltpu.CompilerParams(vmem_limit_bytes=60 << 20),
        cost_estimate=pl.CostEstimate(flops=flops, bytes_accessed=2 * size * (size + 2 * width), transcendentals=0),
    )(packed, v)


def on_device(up_weight, up_momentum, up_grads, out_weight, out_momentum, out_grads):
    even = lax.axis_index("rep") % 2 == 0
    up_moment = MOMENT * up_momentum + reduced_grad(up_grads[0])
    out_moment = MOMENT * out_momentum + reduced_grad(out_grads[0])
    up = to_columns(up_moment.astype(BF))
    out = to_columns(out_moment.astype(BF))
    width, narrow = up.shape[1], out.shape[1]
    out = jnp.pad(out, ((0, 0), (0, width - narrow)))
    other = swap_pairs(jnp.where(even, out, up))
    values = jnp.concatenate([jnp.where(even, up, out), other], axis=1)
    final = chain(total_gram(gram(values)), values)
    mine, other = final[:, :width], swap_pairs(final[:, width:])
    up = to_rows(jnp.where(even, mine, other)).astype(F32)
    out = to_rows(jnp.where(even, other, mine)[:, :narrow]).astype(F32)
    group = lax.axis_size("tp") * lax.axis_size("rep")
    up_direction = up * math.sqrt(up_weight.shape[1] * group)
    out_direction = out * math.sqrt(out_weight.shape[1] * group)
    return (
        up_weight - RATE * up_direction,
        up_moment,
        up_direction,
        out_weight - RATE * out_direction,
        out_moment,
        out_direction,
    )


def solution(mesh):
    flat = P("fs", ("tp", "rep"))
    grads = P("rep", "fs", "tp")
    return jax.shard_map(
        on_device,
        mesh=mesh,
        in_specs=(flat, flat, grads, flat, flat, grads),
        out_specs=(flat,) * 6,
        check_vma=False,
    )
```

```python
import functools
import math

import jax
import jax.numpy as jnp
from jax import lax
from jax.experimental import pallas as pl
from jax.experimental.pallas import tpu as pltpu
from jax.sharding import PartitionSpec as P

ITERS = 3
MOMENT = 0.9
RATE = 0.02
COEF_A = 3.4445
COEF_B = -4.775
COEF_C = 2.0315
BF = jnp.bfloat16
F32 = jnp.float32
CUTS = 8
PANELS = 4


def mm(a, b):
    return jnp.dot(a, b, preferred_element_type=F32)


def mm_t(a, b):
    return lax.dot_general(a, b, (((1,), (1,)), ((), ())), preferred_element_type=F32)


def reduced_grad(grads):
    size = lax.axis_size("rep")
    rows, cols = grads.shape
    pieces = grads.reshape(rows, size, cols // size).transpose(1, 0, 2)
    pieces = lax.all_to_all(pieces, "rep", split_axis=0, concat_axis=0, tiled=True)
    return jnp.sum(pieces.astype(F32), axis=0)


def to_columns(values):
    size = lax.axis_size("fs")
    rows, cols = values.shape
    pieces = values.reshape(rows, size, cols // size).transpose(1, 0, 2)
    pieces = lax.all_to_all(pieces, "fs", split_axis=0, concat_axis=0, tiled=True)
    return pieces.reshape(size * rows, cols // size)


def to_rows(values):
    size = lax.axis_size("fs")
    rows, cols = values.shape
    pieces = values.reshape(size, rows // size, cols)
    pieces = lax.all_to_all(pieces, "fs", split_axis=0, concat_axis=0, tiled=True)
    return pieces.transpose(1, 0, 2).reshape(rows // size, cols * size)


def swap_pairs(values):
    size = lax.axis_size("rep")
    return lax.ppermute(values, "rep", [(i, i ^ 1) for i in range(size)])


def blocks_of(cuts):
    return [(i, j) for i in range(cuts) for j in range(i, cuts)]


def gram_kernel(x_ref, o_ref):
    step = x_ref.shape[0] // CUTS
    span = CUTS // PANELS
    place = {pair: k for k, pair in enumerate(blocks_of(CUTS))}
    for p in range(PANELS):
        low = p * span
        rows = x_ref[low * step : (low + span) * step, :]
        value = mm_t(rows, x_ref[low * step :, :]).astype(BF)
        for i in range(span):
            for j in range(low + i, CUTS):
                k = place[low + i, j]
                o_ref[k * step : (k + 1) * step, :] = value[
                    i * step : (i + 1) * step, (j - low) * step : (j - low + 1) * step
                ]


def grams_kernel(xu, xo, o_ref, v_ref, whole, sem):
    t, r = lax.axis_index("tp"), lax.axis_index("rep")
    width = v_ref.shape[1]

    @pl.when(r == 0)
    def _():
        gram_kernel(xu, o_ref)
        v_ref[...] = xu[...]

    @pl.when(r == 1)
    def _():
        load = pltpu.make_async_copy(xo, whole, sem)
        load.start()
        load.wait()
        gram_kernel(whole, o_ref)
        v_ref[...] = whole[:, pl.ds(pl.multiple_of(t * width, width), width)]


def packed_shape(size):
    return jax.ShapeDtypeStruct((len(blocks_of(CUTS)) * (size // CUTS), size // CUTS), BF)


def gram(x):
    size, width = x.shape
    packed = packed_shape(size)
    return pl.pallas_call(
        gram_kernel,
        name="gram",
        out_shape=packed,
        in_specs=[pl.BlockSpec(memory_space=pltpu.VMEM)],
        out_specs=pl.BlockSpec(memory_space=pltpu.VMEM),
        compiler_params=pltpu.CompilerParams(vmem_limit_bytes=48 << 20),
        cost_estimate=pl.CostEstimate(
            flops=2 * width * math.prod(packed.shape), bytes_accessed=2 * size * width, transcendentals=0
        ),
    )(x)


def grams(xu, xo):
    size, width = xu.shape
    packed = packed_shape(size)
    vmem = pl.BlockSpec(memory_space=pltpu.VMEM)
    return pl.pallas_call(
        grams_kernel,
        name="grams",
        out_shape=[packed, jax.ShapeDtypeStruct(xu.shape, BF)],
        in_specs=[vmem, pl.BlockSpec(memory_space=pl.ANY)],
        out_specs=[vmem, vmem],
        scratch_shapes=[pltpu.VMEM(xo.shape, BF), pltpu.SemaphoreType.DMA],
        compiler_params=pltpu.CompilerParams(vmem_limit_bytes=48 << 20),
        cost_estimate=pl.CostEstimate(
            flops=2 * size * math.prod(packed.shape), bytes_accessed=2 * size * size, transcendentals=0
        ),
    )(xu, xo)


MESH = pl.DeviceIdType.MESH


def greet(peers):
    barrier = pltpu.get_barrier_semaphore()
    for peer in peers:
        pl.semaphore_signal(barrier, inc=1, device_id=peer, device_id_type=MESH)
    pl.semaphore_wait(barrier, len(peers))


class Copies:
    def __init__(self, send, recv, anyone):
        self.send, self.recv, self.anyone, self.started = send, recv, anyone, []

    def make(self, key, src, dst, peer):
        return pltpu.make_async_remote_copy(
            src_ref=src,
            dst_ref=dst,
            send_sem=self.send.at[key],
            recv_sem=self.recv.at[key],
            device_id=peer,
            device_id_type=MESH,
        )

    def start(self, key, src, dst, peer):
        copy = self.make(key, src, dst, peer)
        copy.start()
        self.started.append(copy)

    def arrived(self, key, dst):
        self.make(key, dst, dst, self.anyone).wait_recv()

    def sent(self):
        for copy in self.started:
            copy.wait_send()
        self.started = []


S1X, S1Y, S2X0, S2X1, S2Y0, S2Y1, RZ, AZ, AX, AY, AD0, AD1 = range(12)


class Spread:
    def __init__(self, copies, at, planes, z, t, r):
        self.copies, self.at, self.planes = copies, at, planes
        self.z, self.t, self.r = z, t, r
        self.to_x, self.to_y = (z, t ^ 1, r), (z, t ^ 2, r)

    def to_neighbours(self, m):
        place = self.at(m, self.t, None)
        self.copies.start((AX, m), place, place, self.to_x)
        self.copies.start((AY, m), place, place, self.to_y)

    def to_corner(self, m):
        self.copies.arrived((AX, m), self.at(m, self.t ^ 1, None))
        place = self.at(m, self.t ^ 1, 0)
        self.copies.start((AD0, m), place, place, self.to_y)
        self.copies.arrived((AY, m), self.at(m, self.t ^ 2, None))
        place = self.at(m, self.t ^ 2, 1)
        self.copies.start((AD1, m), place, place, self.to_x)

    def along(self):
        place = self.at(0, self.t, None)
        for m in range(1, self.planes):
            self.copies.start((AZ, m), place, place, (self.z ^ m, self.t, self.r))

    def rest(self):
        before = 0
        for m in range(1, self.planes):
            self.copies.arrived((AZ, m), self.at(m, self.t, None))
            self.to_neighbours(m)
            self.to_corner(before)
            before = m
        self.to_corner(before)
        for m in range(self.planes):
            self.copies.arrived((AD0, m), self.at(m, self.t ^ 3, 0))
            self.copies.arrived((AD1, m), self.at(m, self.t ^ 3, 1))


def reduce_kernel(planes, g_ref, o_ref, first, second, mixed, third, moved, own, send, recv):
    z, t, r = lax.axis_index("fs"), lax.axis_index("tp"), lax.axis_index("rep")
    half = g_ref.shape[1] // 2
    parts = (pl.ds(0, half), pl.ds(half, half))
    beside, above, corner = t ^ 1, t ^ 2, t ^ 3
    to_x, to_y = (z, beside, r), (z, above, r)
    others = list(range(1, planes))
    order = others + [0]
    greet([to_x, to_y] + [(z ^ m, t, r) for m in others])

    def chunk(m, s):
        return (z ^ m) * 4 + s

    @pl.when(r == 1)
    def _():
        o_ref[...] = g_ref[...]

    @pl.when(r == 0)
    def _():
        copies = Copies(send, recv, to_x)

        def corner_halves(m):
            copies.start((S1Y, m), g_ref.at[chunk(m, corner), parts[0]], first.at[m, 0], to_y)
            copies.start((S1X, m), g_ref.at[chunk(m, corner), parts[1]], first.at[m, 1], to_x)

        def direct_halves(m):
            copies.start((S2X1, m), g_ref.at[chunk(m, beside), parts[1]], second.at[m, 0, parts[1]], to_x)
            copies.start((S2Y0, m), g_ref.at[chunk(m, above), parts[0]], second.at[m, 1, parts[0]], to_y)

        corner_halves(order[0])
        corner_halves(order[1])
        direct_halves(order[0])
        for k in range(planes + 1):
            if k < planes:
                m = order[k]
                copies.arrived((S1Y, m), first.at[m, 0])
                mixed[m, 0] = (g_ref[chunk(m, beside), parts[0]].astype(F32) + first[m, 0].astype(F32)).astype(BF)
                copies.start((S2X0, m), mixed.at[m, 0], second.at[m, 0, parts[0]], to_x)
                copies.arrived((S1X, m), first.at[m, 1])
                mixed[m, 1] = (g_ref[chunk(m, above), parts[1]].astype(F32) + first[m, 1].astype(F32)).astype(BF)
                copies.start((S2Y1, m), mixed.at[m, 1], second.at[m, 1, parts[1]], to_y)
                if k + 2 < planes:
                    corner_halves(order[k + 2])
                if k + 1 < planes:
                    direct_halves(order[k + 1])
            if k >= 1:
                m = order[k - 1]
                copies.arrived((S2X1, m), second.at[m, 0, parts[1]])
                copies.arrived((S2Y0, m), second.at[m, 1, parts[0]])
                copies.arrived((S2X0, m), second.at[m, 0, parts[0]])
                copies.arrived((S2Y1, m), second.at[m, 1, parts[1]])
                value = g_ref[chunk(m, t)].astype(F32) + second[m, 0].astype(F32) + second[m, 1].astype(F32)
                if m:
                    moved[m] = value.astype(BF)
                    copies.start((RZ, m), moved.at[m], third.at[m], (z ^ m, t, r))
                else:
                    own[...] = value
        value = own[...]
        for m in others:
            copies.arrived((RZ, m), third.at[m])
            value = value + third[m].astype(F32)
        o_ref[chunk(0, t)] = value.astype(BF)

        def at(m, s, which):
            place = o_ref.at[chunk(m, s)]
            return place if which is None else place.at[parts[which]]

        spread = Spread(copies, at, planes, z, t, r)
        spread.to_neighbours(0)
        spread.along()
        spread.rest()
        copies.sent()


def reduced(packed):
    planes = lax.axis_size("fs")
    chunks = planes * 4
    rows, width = packed.shape
    size = rows // chunks
    out = pl.pallas_call(
        functools.partial(reduce_kernel, planes),
        name="reduced",
        out_shape=jax.ShapeDtypeStruct((chunks, size, width), BF),
        in_specs=[pl.BlockSpec(memory_space=pltpu.VMEM)],
        out_specs=pl.BlockSpec(memory_space=pltpu.VMEM),
        scratch_shapes=[
            pltpu.VMEM((planes, 2, size // 2, width), BF),
            pltpu.VMEM((planes, 2, size, width), BF),
            pltpu.VMEM((planes, 2, size // 2, width), BF),
            pltpu.VMEM((planes, size, width), BF),
            pltpu.VMEM((planes, size, width), BF),
            pltpu.VMEM((size, width), F32),
            pltpu.SemaphoreType.DMA((12, planes)),
            pltpu.SemaphoreType.DMA((12, planes)),
        ],
        compiler_params=pltpu.CompilerParams(
            collective_id=1, has_side_effects=True, vmem_limit_bytes=48 << 20
        ),
    )(packed.reshape(chunks, size, width))
    return out.reshape(rows, width)


def front_kernel(
    planes, um, ug, om, og, up_moment, out_moment, xu, xo, gu, go, mine, block, send, recv, pair_send, pair_recv,
    up_send, up_recv, local,
):
    z, t, r = lax.axis_index("fs"), lax.axis_index("tp"), lax.axis_index("rep")
    rows, cols = um.shape
    narrow = om.shape[1]
    step = cols // planes
    partner = (z, t, 1 - r)
    others = list(range(1, planes))
    greet(
        [partner, (z, t ^ 1, r), (z, t ^ 2, r)]
        + [(z ^ m, t, c) for m in others for c in range(2)]
    )
    order = others[::-1] + [0]

    def span(start, size):
        return pl.ds(pl.multiple_of(start, size), size)

    pairs = Copies(pair_send, pair_recv, partner)
    for m in order:
        pairs.start((m,), ug.at[:, span((1 - r) * cols + (z ^ m) * step, step)], gu.at[m], partner)
    pairs.start((planes,), og.at[:, span((1 - r) * narrow, narrow)], go, partner)

    ups = Copies(up_send, up_recv, partner)
    target = xu.at[span(z * rows, rows), span(r * step, step)]
    for m in order:
        pairs.arrived((m,), gu.at[m])
        place = span((z ^ m) * step, step)
        grad = ug[:, span(r * cols + (z ^ m) * step, step)].astype(F32) + gu[m].astype(F32)
        value = MOMENT * um[:, place] + grad
        up_moment[:, place] = value
        mine[m] = value.astype(BF)
        if m:
            for c in range(2):
                @pl.when(r == c)
                def _(m=m, c=c):
                    ups.make((m, c), mine.at[m], target, (z ^ m, t, 0)).start()
        else:
            @pl.when(r == 1)
            def _(m=m):
                ups.make((0, 1), mine.at[m], target, (z, t, 0)).start()

            @pl.when(r == 0)
            def _(m=m):
                xu[span(z * rows, rows), span(0, step)] = mine[m]

    pairs.arrived((planes,), go)
    grad = og[:, span(r * narrow, narrow)].astype(F32) + go[...].astype(F32)
    value = MOMENT * om[...] + grad
    out_moment[...] = value
    block[...] = value.astype(BF)

    def at(m, s, which):
        first = s * 2 * narrow
        if which is None:
            return xo.at[span((z ^ m) * rows, rows), span(first, 2 * narrow)]
        return xo.at[span((z ^ m) * rows, rows), span(first + which * narrow, narrow)]

    def up_sent(c):
        for m in order:
            if m or c:
                ups.make((m, c), mine.at[m], target, partner).wait_send()

    @pl.when(r == 0)
    def _():
        copies = Copies(pair_send, pair_recv, partner)
        copies.start((planes + 1,), block, at(0, t, 0), partner)
        for m in order:
            for c in range(2):
                if m or c:
                    place = xu.at[span((z ^ m) * rows, rows), span(c * step, step)]
                    ups.arrived((m, c), place)
        up_sent(0)
        copies.sent()

    @pl.when(r == 1)
    def _():
        keep = pltpu.make_async_copy(block, at(0, t, 1), local)
        keep.start()
        keep.wait()
        pairs.arrived((planes + 1,), at(0, t, 0))
        copies = Copies(send, recv, partner)
        spread = Spread(copies, at, planes, z, t, r)
        spread.to_neighbours(0)
        up_sent(1)
        spread.along()
        spread.rest()
        copies.sent()

    pairs.sent()


def front(um, ug, om, og):
    planes = lax.axis_size("fs")
    rows, cols = um.shape
    narrow = om.shape[1]
    step = cols // planes
    vmem = pl.BlockSpec(memory_space=pltpu.VMEM)
    return pl.pallas_call(
        functools.partial(front_kernel, planes),
        name="front",
        out_shape=[
            jax.ShapeDtypeStruct(um.shape, F32),
            jax.ShapeDtypeStruct(om.shape, F32),
            jax.ShapeDtypeStruct((planes * rows, 2 * step), BF),
            jax.ShapeDtypeStruct((planes * rows, 8 * narrow), BF),
        ],
        in_specs=[vmem] * 4,
        out_specs=[vmem] * 3 + [pl.BlockSpec(memory_space=pl.ANY)],
        scratch_shapes=[
            pltpu.VMEM((planes, rows, step), BF),
            pltpu.VMEM((rows, narrow), BF),
            pltpu.VMEM((planes, rows, step), BF),
            pltpu.VMEM((rows, narrow), BF),
            pltpu.SemaphoreType.DMA((12, planes)),
            pltpu.SemaphoreType.DMA((12, planes)),
            pltpu.SemaphoreType.DMA((planes + 2,)),
            pltpu.SemaphoreType.DMA((planes + 2,)),
            pltpu.SemaphoreType.DMA((planes, 2)),
            pltpu.SemaphoreType.DMA((planes, 2)),
            pltpu.SemaphoreType.DMA,
        ],
        compiler_params=pltpu.CompilerParams(
            collective_id=2, has_side_effects=True, vmem_limit_bytes=56 << 20
        ),
    )(um, ug, om, og)


def back_kernel(planes, v_ref, ub, ob, up_send, up_recv, out_send, out_recv):
    z, t, r = lax.axis_index("fs"), lax.axis_index("tp"), lax.axis_index("rep")
    rows, cols = ub.shape
    step = cols // planes
    narrow = ob.shape[1]
    partner = (z, t, 1 - r)
    others = list(range(1, planes))
    greet([partner] + [(z ^ m, t, c) for m in others for c in range(2)])

    def span(start, size):
        return pl.ds(pl.multiple_of(start, size), size)

    ups = Copies(up_send, up_recv, partner)
    outs = Copies(out_send, out_recv, partner)
    target = ub.at[:, span(z * step, step)]

    def piece(m, c):
        return v_ref.at[span((z ^ m) * rows, rows), pl.ds(c * step, step)]

    @pl.when(r == 0)
    def _():
        for m in others[::-1] + [0]:
            for c in range(2):
                if m or c:
                    pltpu.make_async_remote_copy(
                        src_ref=piece(m, c), dst_ref=target, send_sem=up_send.at[m, c], recv_sem=up_recv.at[m, 0],
                        device_id=(z ^ m, t, c), device_id_type=MESH,
                    ).start()
        ub[:, span(z * step, step)] = v_ref[span(z * rows, rows), pl.ds(0, step)]
        outs.arrived((0,), ob)

    @pl.when(r == 1)
    def _():
        outs.start((0,), v_ref.at[span(z * rows, rows), pl.ds(0, narrow)], ob, partner)
        ob[...] = v_ref[span(z * rows, rows), pl.ds(narrow, narrow)]
        ups.arrived((0, 0), target)
        outs.sent()

    for m in others:
        ups.arrived((m, 0), ub.at[:, span((z ^ m) * step, step)])

    @pl.when(r == 0)
    def _():
        for m in others[::-1] + [0]:
            for c in range(2):
                if m or c:
                    ups.make((m, c), piece(m, c), target, partner).wait_send()


def back(v, rows, cols, narrow):
    planes = lax.axis_size("fs")
    vmem = pl.BlockSpec(memory_space=pltpu.VMEM)
    return pl.pallas_call(
        functools.partial(back_kernel, planes),
        name="back",
        out_shape=[jax.ShapeDtypeStruct((rows, cols), BF), jax.ShapeDtypeStruct((rows, narrow), BF)],
        in_specs=[vmem],
        out_specs=[vmem] * 2,
        scratch_shapes=[
            pltpu.SemaphoreType.DMA((planes, 2)),
            pltpu.SemaphoreType.DMA((planes, 2)),
            pltpu.SemaphoreType.DMA((1,)),
            pltpu.SemaphoreType.DMA((1,)),
        ],
        compiler_params=pltpu.CompilerParams(
            collective_id=3, has_side_effects=True, vmem_limit_bytes=32 << 20
        ),
    )(v)


def square_of_four(um, om):
    fs, tp, rep = (lax.axis_size(name) for name in ("fs", "tp", "rep"))
    step, blocks = um.shape[1] // fs, len(blocks_of(CUTS))
    size = um.shape[0] * fs
    return (
        rep == 2
        and tp == 4
        and fs > 1
        and fs & (fs - 1) == 0
        and um.shape[0] % 16 == 0
        and step % 128 == 0
        and om.shape[1] == step
        and size == 8 * om.shape[1]
        and blocks * (size // CUTS) % (fs * tp * 32) == 0
    )


def summed(packed):
    rep = lax.axis_size("rep")
    packed = lax.psum(packed, ("fs", "tp"))
    if rep > 2:
        groups = [[i for i in range(rep) if i % 2 == k] for k in range(2)]
        packed = lax.psum(packed, "rep", axis_index_groups=groups)
    return packed


def unpack(packed, mats):
    step = packed.shape[1]
    pairs = blocks_of(CUTS)
    total = jnp.zeros((step, step), F32)
    for k, (i, j) in enumerate(pairs):
        value = packed[k * step : (k + 1) * step, :].astype(F32)
        total = total + (value * value if i == j else 2.0 * (value * value))
    square = 1.0 / (jnp.sqrt(jnp.sum(total, keepdims=True)) + 1.0)
    for k, (i, j) in enumerate(pairs):
        value = (packed[k * step : (k + 1) * step, :].astype(F32) * square).astype(BF)
        mats[0, i * step : (i + 1) * step, j * step : (j + 1) * step] = value
        if i != j:
            mats[0, j * step : (j + 1) * step, i * step : (i + 1) * step] = value.T
    return jnp.sqrt(square)


def symmetric_step(mats, left, right, out, alpha, beta):
    size = mats.shape[1]
    step = size // PANELS
    for i in range(PANELS):
        low, high = i * step, (i + 1) * step
        product = mm(mats[left, low:high, :], mats[right, :, low:])
        value = (alpha * mats[right, low:high, low:].astype(F32) + beta * product).astype(BF)
        mats[out, low:high, low:] = value
        for j in range(i + 1, PANELS):
            mats[out, j * step : (j + 1) * step, low:high] = value[:, (j - i) * step : (j - i + 1) * step].T


def thin_step(mats, index, vals, source, target, alpha):
    size = mats.shape[1]
    step = size // PANELS

    def panel(i, _):
        rows = pl.ds(pl.multiple_of(i * step, step), step)
        product = mm(mats[index, rows, :], vals[source])
        vals[target, rows, :] = (alpha * vals[source, rows, :].astype(F32) + product).astype(BF)
        return 0

    lax.fori_loop(0, PANELS, panel, 0)


def chain_kernel(g_ref, v_ref, o_ref, mats, vals):
    factor = unpack(g_ref, mats)
    vals[0] = v_ref[...]

    def product(k, _):
        left = jnp.where(k == 0, 0, 1)
        right = jnp.where(k == 2, 2, 0)
        out = jnp.where(k == 0, 1, jnp.where(k == 1, 2, 0))
        alpha = jnp.where(k == 0, COEF_B, COEF_A).astype(F32)
        beta = jnp.where(k == 0, COEF_C, 1.0).astype(F32)
        symmetric_step(mats, left, right, out, alpha, beta)
        return 0

    def iteration(t, _):
        lax.fori_loop(0, 3, product, 0)
        thin_step(mats, 1, vals, t, t + 1, COEF_A)
        return 0

    lax.fori_loop(0, ITERS - 1, iteration, 0)
    size = mats.shape[1]
    step = size // PANELS
    last = ITERS - 1
    for source, target in ((last, 0), (0, 1)):
        def panel(i, _):
            rows = pl.ds(pl.multiple_of(i * step, step), step)
            product = mm(mats[0, rows, :], vals[source])
            if target == 0:
                vals[0, rows, :] = product.astype(BF)
            else:
                value = COEF_A * vals[last, rows, :].astype(F32) + COEF_B * vals[0, rows, :].astype(F32)
                o_ref[rows, :] = (factor * (value + COEF_C * product)).astype(BF)
            return 0
        lax.fori_loop(0, PANELS, panel, 0)


def chain(packed, v):
    size, width = v.shape
    flops = 2 * size * size * (4 * width + 6 * size * 5 // 8)
    return pl.pallas_call(
        chain_kernel,
        name="chain",
        out_shape=jax.ShapeDtypeStruct(v.shape, BF),
        in_specs=[pl.BlockSpec(memory_space=pltpu.VMEM)] * 2,
        out_specs=pl.BlockSpec(memory_space=pltpu.VMEM),
        scratch_shapes=[pltpu.VMEM((3, size, size), BF), pltpu.VMEM((ITERS, size, width), BF)],
        compiler_params=pltpu.CompilerParams(vmem_limit_bytes=60 << 20),
        cost_estimate=pl.CostEstimate(flops=flops, bytes_accessed=2 * size * (size + 2 * width), transcendentals=0),
    )(packed, v)


def by_kernels(up_momentum, up_grads, out_momentum, out_grads):
    up_moment, out_moment, xu, xo = front(up_momentum, up_grads, out_momentum, out_grads)
    packed, values = grams(xu, xo)
    final = chain(reduced(packed), values)
    up, out = back(final, *up_momentum.shape, out_momentum.shape[1])
    return up_moment, out_moment, up, out


def by_collectives(up_momentum, up_grads, out_momentum, out_grads):
    even = lax.axis_index("rep") % 2 == 0
    up_moment = MOMENT * up_momentum + reduced_grad(up_grads)
    out_moment = MOMENT * out_momentum + reduced_grad(out_grads)
    up = to_columns(up_moment.astype(BF))
    out = to_columns(out_moment.astype(BF))
    width, narrow = up.shape[1], out.shape[1]
    out = jnp.pad(out, ((0, 0), (0, width - narrow)))
    other = swap_pairs(jnp.where(even, out, up))
    values = jnp.concatenate([jnp.where(even, up, out), other], axis=1)
    final = chain(summed(gram(values)), values)
    mine, other = final[:, :width], swap_pairs(final[:, width:])
    up = to_rows(jnp.where(even, mine, other))
    out = to_rows(jnp.where(even, other, mine)[:, :narrow])
    return up_moment, out_moment, up, out


def on_device(up_weight, up_momentum, up_grads, out_weight, out_momentum, out_grads):
    way = by_kernels if square_of_four(up_momentum, out_momentum) else by_collectives
    up_moment, out_moment, up, out = way(up_momentum, up_grads[0], out_momentum, out_grads[0])
    group = lax.axis_size("tp") * lax.axis_size("rep")
    up_direction = up.astype(F32) * math.sqrt(up_weight.shape[1] * group)
    out_direction = out.astype(F32) * math.sqrt(out_weight.shape[1] * group)
    return (
        up_weight - RATE * up_direction,
        up_moment,
        up_direction,
        out_weight - RATE * out_direction,
        out_moment,
        out_direction,
    )


def solution(mesh):
    flat = P("fs", ("tp", "rep"))
    grads = P("rep", "fs", "tp")
    return jax.shard_map(
        on_device,
        mesh=mesh,
        in_specs=(flat, flat, grads, flat, flat, grads),
        out_specs=(flat,) * 6,
        check_vma=False,
    )
```
